32 devices in a mesh: grp: 2 (over y), sp: 4 (over z), tp: 4 (over x, core).
Axes of the slice: x: 2, y: 2, z: 4, core: 2. Of those that a mesh axis runs over, the one named last changes fastest.
Arguments:
- tokens: bfloat16 [1280, 2048], P(('grp', 'sp')), parts along dimension 0, may hold values from -6 to 6
- norm_gain: float32 [2048], replicated, may hold values from 0.6 to 5
- query_weight: bfloat16 [2048, 2048], P('sp', 'tp')
- key_weight: bfloat16 [2048, 512], P('sp', 'tp')
- value_weight: bfloat16 [2048, 512], P('sp', 'tp'), may hold values from -0.125 to 0.125
- map_lambda: float32 [16], P('tp'), may hold values from 0.3 to 0.8
- head_gain: float32 [16, 128], P('tp'), may hold values from 0.1 to 1.9
- attn_out_weight: bfloat16 [2048, 2048], P('tp', 'sp'), may hold values from -0.125 to 0.125
- pool_out_weight: bfloat16 [2048, 2048], P('tp', 'sp'), may hold values from -0.09375 to 0.09375
Outputs:
- mixed_rows: bfloat16 [1280, 2048], P(('grp', 'sp', 'tp')), parts along dimension 0
- log_totals: float32 [2, 16, 1280], P(None, 'tp', ('grp', 'sp')), parts along dimension 2
The draws below stay inside these ranges and needn't reach their ends.
There are 2 independent parts, one for each index of `grp`. The reference program is written for one: setup_inputs(seed, part) draws one part's arguments, and reference() takes and returns one part's arrays. A program takes and returns all parts, laid end to end along the dimension named above; an argument that names none is the same for every part. Nothing has to cross between parts.
All inputs are finite; a program needn't handle non-finite values.
Results may differ from the reference program's by a relative error of at most 0.013.
The reference program's roundings to bfloat16 on the way (of `normed`, `head_rows` and `pooled`) count: a program that leaves them out, or rounds other values in their place, can miss the bound.
Values may be sent and summed in bfloat16 or wider, within the bound.
A program may use at most 64 MiB of HBM per device.

```python
import math
import jax
import jax.numpy as jnp
from jax import lax

D = 2048
HEADS = 16
KV_HEADS = 4
HD = 64
VD = 128
SEQ = 640


def projection_pair(key):
    base_key = jax.random.fold_in(key, 71)
    query_key, other_key = jax.random.split(base_key)
    spread_std = 1.32 / math.sqrt(D)
    w_query = jax.random.normal(query_key, (D, HEADS * 2 * HD), jnp.float32) * spread_std
    fresh_part = jax.random.normal(other_key, (D, KV_HEADS * 2 * HD), jnp.float32) * spread_std
    w_key = fresh_part
    return (w_query, w_key)


def draw_query_weight(key, part):
    return projection_pair(key)[0].astype(jnp.bfloat16)


def draw_key_weight(key, part):
    return projection_pair(key)[1].astype(jnp.bfloat16)


def draw_norm_gain(key, part):
    gain_key = jax.random.fold_in(key, 13)
    return jax.random.uniform(gain_key, (D,), jnp.float32, 0.6, 1.4)


def shard_levels(own_key, shape, cuts, least, top_value):
    level, own = 1.0, jax.random.fold_in(own_key, 6)
    for dim, shards_of in cuts:
        steps = jnp.exp(jax.random.uniform(jax.random.fold_in(own, dim), (shards_of,), jnp.float32, least / len(cuts), top_value / len(cuts)))
        level = level * jnp.repeat(steps, shape[dim] // shards_of).reshape([-1 if axis == dim else 1 for axis in range(len(shape))])
    return level


def scatter_about(stream_key, dims, deviation, limit, cuts=(), kind=jnp.bfloat16):
    values = deviation * jax.random.normal(stream_key, dims, jnp.float32)
    if cuts:
        values = values * shard_levels(stream_key, dims, cuts, -0.22, 0.18)
    return jnp.clip(values, -limit, limit).astype(kind)


def setup_inputs(seed: int = 0, part: int = 0) -> dict:
    streams_of = jax.random.split(jax.random.key(seed), 10)
    part_splits = jax.random.split(jax.random.fold_in(streams_of[9], part), 10)
    tokens = scatter_about(part_splits[0], (SEQ, D), 1.0, 6.0, ((0, 4),))
    norm_gain = draw_norm_gain(jax.random.fold_in(streams_of[9], 71), part)
    query_weight = draw_query_weight(jax.random.fold_in(streams_of[9], 71), part)
    key_weight = draw_key_weight(jax.random.fold_in(streams_of[9], 71), part)
    value_weight = scatter_about(streams_of[4], (D, KV_HEADS * VD), D ** -0.5, 0.125, ((0, 4), (1, 4)))
    map_lambda = jnp.clip(0.3 + 0.5 * jax.random.uniform(streams_of[5], (HEADS,), jnp.float32) ** shard_levels(streams_of[5], (HEADS,), ((0, 4),), -0.2, 0.2), 0.3, 0.8)
    head_gain = jnp.clip(1.0 + 0.18 * jax.random.normal(streams_of[6], (HEADS, VD), jnp.float32), 0.1, 1.9)
    attn_out_weight = scatter_about(streams_of[7], (HEADS * VD, D), (HEADS * VD) ** -0.5, 0.125, ((0, 4), (1, 4)))
    pool_out_weight = scatter_about(streams_of[8], (D, D), (2 * D) ** -0.5, 0.09375, ((0, 4), (1, 4)))
    return {"tokens": tokens, "norm_gain": norm_gain, "query_weight": query_weight, "key_weight": key_weight, "value_weight": value_weight, "map_lambda": map_lambda, "head_gain": head_gain, "attn_out_weight": attn_out_weight, "pool_out_weight": pool_out_weight}


epsilon = 1e-06

def reference(tokens, norm_gain, query_weight, key_weight, value_weight, map_lambda, head_gain, attn_out_weight, pool_out_weight):
    group_heads = HEADS // KV_HEADS
    tokens_wide = tokens.astype(jnp.float32)
    normed = (tokens_wide * lax.rsqrt(lax.optimization_barrier(jnp.mean(tokens_wide * tokens_wide, axis=-1, keepdims=True)) + epsilon) * norm_gain).astype(jnp.bfloat16)
    queries = jnp.dot(normed, query_weight, preferred_element_type=jnp.float32).astype(jnp.bfloat16)
    keys = jnp.dot(normed, key_weight, preferred_element_type=jnp.float32).astype(jnp.bfloat16)
    values = jnp.dot(normed, value_weight, preferred_element_type=jnp.float32).astype(jnp.bfloat16)
    keys_f32 = keys.reshape(SEQ, KV_HEADS, 2, HD).astype(jnp.float32)
    values_f32 = values.reshape(SEQ, KV_HEADS, VD).astype(jnp.float32)
    block_len = math.gcd(SEQ, 256)
    query_blocks = queries.reshape(SEQ // block_len, block_len, KV_HEADS, group_heads, 2, HD)
    lambdas = map_lambda.reshape(KV_HEADS, group_heads, 1, 1)
    gains = head_gain.reshape(KV_HEADS, group_heads, 1, VD)

    def attend(query_blk):
        scores = jnp.einsum('qhgmd,khmd->hgmqk', query_blk.astype(jnp.float32), keys_f32) * HD ** (-0.5)
        highest = lax.optimization_barrier(jnp.max(scores, axis=-1))
        weights = jnp.exp(scores - highest[..., None])
        totals = lax.optimization_barrier(jnp.sum(weights, axis=-1))
        weights_b = lax.optimization_barrier(weights.astype(jnp.bfloat16)).astype(jnp.float32)
        reads = jnp.einsum('hgmqk,khe->hgmqe', weights_b, values_f32) / totals[..., None]
        contrast = reads[:, :, 0] - lambdas * reads[:, :, 1]
        scaled = contrast * lax.rsqrt(lax.optimization_barrier(jnp.mean(contrast * contrast, axis=-1, keepdims=True)) + epsilon) * gains
        head_rows = jnp.transpose(scaled, (2, 0, 1, 3)).reshape(block_len, HEADS * VD)
        return (head_rows.astype(jnp.bfloat16), highest + jnp.log(totals))
    head_rows, log_parts = lax.map(attend, query_blocks)
    head_rows = head_rows.reshape(SEQ, HEADS * VD)
    log_totals = jnp.transpose(log_parts, (3, 1, 2, 0, 4)).reshape(2, HEADS, SEQ)
    normed_f32 = normed.astype(jnp.float32)
    prefix = jnp.concatenate([jnp.zeros((1, D), jnp.float32), jnp.cumsum(normed_f32, axis=0)], axis=0)
    position = jnp.arange(SEQ)
    group_width = D // 4
    pieces = []
    for group in range(4):
        window = 2 ** (group + 1)
        lower_edge = jnp.clip(position - window // 2, 0, SEQ)
        upper_edge = jnp.clip(position + window - window // 2, 0, SEQ)
        counts_f = (upper_edge - lower_edge).astype(jnp.float32)[:, None]
        columns = prefix[:, group * group_width:(group + 1) * group_width]
        own_chan = normed_f32[:, group * group_width:(group + 1) * group_width]
        pieces.append((columns[upper_edge] - columns[lower_edge]) / counts_f - own_chan)
    pooled = jnp.concatenate(pieces, axis=1).astype(jnp.bfloat16)
    mixed = jnp.dot(head_rows, attn_out_weight, preferred_element_type=jnp.float32) + jnp.dot(pooled, pool_out_weight, preferred_element_type=jnp.float32)
    return (mixed.astype(jnp.bfloat16), log_totals)
```

```python
import functools
import math

import jax
import jax.numpy as jnp
from jax import lax
from jax.experimental import pallas as pl
from jax.experimental.pallas import tpu as pltpu
from jax.sharding import PartitionSpec as P

HD = 64
VD = 128
POOL_SPAN = 16


epsilon = 1e-06
very_low = -1e30


def extended(cells, sides, width):
    for axis, dim in sides:
        count = lax.axis_size(axis)
        ends = count - 1
        head = lax.slice_in_dim(cells, 0, width, axis=dim)
        tail = lax.slice_in_dim(cells, cells.shape[dim] - width, cells.shape[dim], axis=dim)
        cells = jnp.concatenate(
            [
                lax.ppermute(tail, axis, [(i, (i + 1) % count) for i in range(ends)]),
                cells,
                lax.ppermute(head, axis, [((i + 1) % count, i) for i in range(ends)]),
            ],
            axis=dim,
        )
    return cells


def add_products(totals, pieces, source):
    results = []
    for running, piece in zip(totals, pieces):
        results.append(jnp.dot(source, piece, preferred_element_type=jnp.float32))
    return tuple(results)


def on_device(
    tokens,
    norm_gain,
    query_weight,
    key_weight,
    value_weight,
    map_lambda,
    head_gain,
    attn_out_weight,
    pool_out_weight,
):
    tokens_wide = tokens.astype(jnp.float32)
    normed = (
        tokens_wide
        * lax.rsqrt(jnp.mean(tokens_wide * tokens_wide, axis=-1, keepdims=True) + epsilon)
        * norm_gain
    ).astype(jnp.bfloat16)
    row_count = normed.shape[0]
    sp_index = lax.axis_index("sp")
    tp_index = lax.axis_index("tp")
    group_width = pool_out_weight.shape[0]
    local_heads = map_lambda.shape[0]
    key_heads = value_weight.shape[1] // VD
    group_heads = local_heads // key_heads
    q_empty = jnp.zeros((row_count, query_weight.shape[1]), jnp.float32)
    k_empty = jnp.zeros((row_count, key_weight.shape[1]), jnp.float32)
    v_empty = jnp.zeros((row_count, value_weight.shape[1]), jnp.float32)
    q_acc, k_acc, v_acc = add_products(
        (q_empty, k_empty, v_empty),
        (
            lax.all_gather(query_weight, "sp", axis=0, tiled=True),
            lax.all_gather(key_weight, "sp", axis=0, tiled=True),
            lax.all_gather(value_weight, "sp", axis=0, tiled=True),
        ),
        normed,
    )
    queries = q_acc.astype(jnp.bfloat16).reshape(row_count, key_heads, group_heads, 2, HD)
    keys_flat = k_acc.astype(jnp.bfloat16)
    values_flat = v_acc.astype(jnp.bfloat16)

    def key_block(state_now, key_pair):
        maxima, totals, accums = state_now
        key_blk, val_blk = key_pair
        scores = jnp.einsum(
            "qhgmd,khmd->hgmqk", queries, key_blk, preferred_element_type=jnp.float32
        ) * HD ** (-0.5)
        highest = jnp.maximum(maxima, jnp.max(scores, axis=-1))
        factor = jnp.exp(maxima - highest)
        weights = jnp.exp(scores - highest[..., None])
        totals = totals * factor + jnp.sum(weights, axis=-1)
        accums = accums * factor[..., None] + jnp.einsum(
            "hgmqk,khe->hgmqe",
            weights.astype(jnp.bfloat16),
            val_blk,
            preferred_element_type=jnp.float32,
        )
        return ((highest, totals, accums), None)

    start_state = (
        jnp.full((key_heads, group_heads, 2, row_count), very_low, jnp.float32),
        jnp.zeros((key_heads, group_heads, 2, row_count), jnp.float32),
        jnp.zeros((key_heads, group_heads, 2, row_count, VD), jnp.float32),
    )
    key_piece = lax.all_gather(keys_flat, "sp", axis=0, tiled=True)
    val_piece = lax.all_gather(values_flat, "sp", axis=0, tiled=True)
    piece_len = key_piece.shape[0]
    block_len = math.gcd(piece_len, 512)
    key_blocks = key_piece.reshape(piece_len // block_len, block_len, key_heads, 2, HD)
    val_blocks = val_piece.reshape(piece_len // block_len, block_len, key_heads, VD)
    state_next, unused = lax.scan(key_block, start_state, (key_blocks, val_blocks))
    maxima, totals, accums = state_next
    log_parts = maxima + jnp.log(totals)
    log_totals = jnp.transpose(log_parts, (2, 0, 1, 3)).reshape(2, local_heads, row_count)
    reads = accums / totals[..., None]
    contrast = reads[:, :, 0] - map_lambda.reshape(key_heads, group_heads, 1, 1) * reads[:, :, 1]
    scaled = (
        contrast
        * lax.rsqrt(jnp.mean(contrast * contrast, axis=-1, keepdims=True) + epsilon)
        * head_gain.reshape(key_heads, group_heads, 1, VD)
    )
    attention_head_rows = (
        jnp.transpose(scaled, (2, 0, 1, 3))
        .reshape(row_count, local_heads * VD)
        .astype(jnp.bfloat16)
    )
    head_rows, log_totals = (attention_head_rows, log_totals)
    own_chan = lax.dynamic_slice_in_dim(normed, tp_index * group_width, group_width, 1)
    reach = POOL_SPAN // 2
    padded = extended(own_chan, (("sp", 0),), reach)
    window = jnp.left_shift(jnp.int32(2), tp_index)
    half_span = window // 2
    running = jnp.zeros((row_count, group_width), jnp.float32)
    for offset in range(POOL_SPAN):
        piece = lax.dynamic_slice_in_dim(padded, reach - half_span + offset, row_count, 0).astype(
            jnp.float32
        )
        running = running + jnp.where(offset < window, piece, 0.0)
    seq_len = row_count * lax.axis_size("sp")
    position = sp_index * row_count + jnp.arange(row_count, dtype=jnp.int32)
    lower_edge = jnp.clip(position - half_span, 0, seq_len)
    upper_edge = jnp.clip(position + window - half_span, 0, seq_len)
    counts_f = (upper_edge - lower_edge).astype(jnp.float32)[:, None]
    pooled = (running / counts_f - own_chan.astype(jnp.float32)).astype(jnp.bfloat16)
    attn_whole, pool_whole = (
        lax.all_gather(attn_out_weight, "sp", axis=1, tiled=True),
        lax.all_gather(pool_out_weight, "sp", axis=1, tiled=True),
    )
    mixed = lax.psum_scatter(
        (
            jnp.dot(head_rows, attn_whole, preferred_element_type=jnp.float32)
            + jnp.dot(pooled, pool_whole, preferred_element_type=jnp.float32)
        ).astype(jnp.bfloat16),
        "tp",
        scatter_dimension=0,
        tiled=True,
    )
    return (mixed, log_totals)


MESH = pl.DeviceIdType.MESH
LANES = 128


def fused_kernel(
    count,
    tok,
    gain,
    wq,
    wk,
    wv,
    lam,
    hgain,
    wao,
    wpo,
    mixed_out,
    lt_out,
    tok_all,
    norm_all,
    w_all,
    q_all,
    k_all,
    v_all,
    heads_all,
    pooled_all,
    part_out,
    part_in,
    block_out,
    block_in,
    lt_send,
    lt_in,
    z_send,
    z_recv,
    f_send,
    f_recv,
    h_send,
    h_recv,
    p_send,
    p_recv,
    o_send,
    o_recv,
    l_send,
    l_recv,
):
    g = lax.axis_index("grp")
    s = lax.axis_index("sp")
    t = lax.axis_index("tp")
    rows, width = tok.shape
    quarter = width // 4
    shard = wq.shape[0]
    half = shard // 2
    sib = t + 1 - 2 * lax.rem(t, 2)
    far = lax.rem(t + 2, 4)
    diag = lax.rem(sib + 2, 4)
    twin = 1 - g
    offs = list(range(1, count))
    order = sorted(offs, key=lambda o: min(o, count - o))
    f32, bf16 = jnp.float32, jnp.bfloat16

    def span(index, size):
        return pl.ds(pl.multiple_of(index * size, size), size)

    def half_rows(owner, part):
        return pl.ds(pl.multiple_of(owner * shard + part * half, half), half)

    barrier = pltpu.get_barrier_semaphore()
    for off in offs:
        pl.semaphore_signal(
            barrier, inc=1, device_id={"sp": lax.rem(s + off, count)}, device_id_type=MESH
        )
    for peer in (sib, far, diag):
        pl.semaphore_signal(barrier, inc=1, device_id={"tp": peer}, device_id_type=MESH)
    pl.semaphore_signal(barrier, inc=1, device_id={"grp": twin}, device_id_type=MESH)
    pl.semaphore_wait(barrier, count - 1 + 4)

    def copy(src, dst, send, recv, where):
        return pltpu.make_async_remote_copy(
            src_ref=src,
            dst_ref=dst,
            send_sem=send,
            recv_sem=recv,
            device_id=where,
            device_id_type=MESH,
        )

    def z_copy(kind, off):
        peer = lax.rem(s + off, count)
        if kind == 0:
            src = tok.at[:, span(t, quarter)]
            dst = tok_all.at[span(s, rows), span(t, quarter)]
        else:
            mine = span(g, half)
            if kind == 1:
                src, col = wk.at[mine, :], 0
            elif kind == 2:
                src, col = wv.at[mine, :], LANES
            else:
                src, col = wq.at[mine, span(peer, LANES)], 2 * LANES
            dst = w_all.at[half_rows(s, g), pl.ds(col, LANES)]
        return copy(src, dst, z_send.at[kind, off], z_recv.at[kind, off], {"sp": peer})

    def tok_forward(step, off):
        owner = lax.rem(s + count - off, count)
        col = span(far if step == 2 else t, quarter)
        place = tok_all.at[span(owner, rows), col]
        where = {"tp": far if step == 1 else sib}
        return copy(place, place, f_send.at[step, off], f_recv.at[step, off], where)

    def w_forward(off):
        owner = lax.rem(s + count - off, count)
        place = w_all.at[half_rows(owner, g), :]
        return copy(place, place, f_send.at[3, off], f_recv.at[3, off], {"grp": twin})

    for kind in range(4):
        for off in order:
            z_copy(kind, off).start()

    def norm_block(ref, base, owner):
        step = 16

        def one(i, carry):
            x = ref[pl.ds(pl.multiple_of(base + i * step, step), step), :].astype(f32)
            scale = lax.rsqrt(jnp.mean(x * x, axis=-1, keepdims=True) + epsilon)
            norm_all[pl.ds(pl.multiple_of(owner * rows + i * step, step), step), :] = (
                x * scale * gain[...]
            ).astype(bf16)
            return carry

        lax.fori_loop(0, rows // step, one, 0)

    w_all[span(s, shard), 0:LANES] = wk[...]
    w_all[span(s, shard), LANES : 2 * LANES] = wv[...]
    w_all[span(s, shard), 2 * LANES : 3 * LANES] = wq[:, span(s, LANES)]
    norm_block(tok, 0, s)

    for off in order:
        z_copy(0, off).wait_recv()
        tok_forward(1, off).start()
        tok_forward(0, off).start()
    for off in order:
        tok_forward(1, off).wait_recv()
        tok_forward(2, off).start()
    for off in order:
        tok_forward(0, off).wait_recv()
        tok_forward(2, off).wait_recv()
        owner = lax.rem(s + count - off, count)
        norm_block(tok_all, owner * rows, owner)

    seq = rows * count
    group = wpo.shape[0]
    window = jnp.where(t == 0, 2, jnp.where(t == 1, 4, jnp.where(t == 2, 8, 16)))
    half_span = window // 2

    def pool(b, carry):
        at = b * rows + lax.broadcasted_iota(jnp.int32, (rows, seq), 0)
        col = lax.broadcasted_iota(jnp.int32, (rows, seq), 1)
        inside = (col >= at - half_span) & (col < at + window - half_span)
        band = jnp.where(inside, 1.0, 0.0).astype(bf16)
        total = jnp.dot(band, norm_all[:, span(t, group)], preferred_element_type=f32)
        pos = b * rows + lax.broadcasted_iota(jnp.int32, (rows, 1), 0)
        low = jnp.maximum(pos - half_span, 0)
        high = jnp.minimum(pos + window - half_span, seq)
        own = norm_all[span(b, rows), span(t, group)].astype(f32)
        pooled_all[span(b, rows), :] = (total / (high - low).astype(f32) - own).astype(bf16)
        return carry

    for off in order:
        for kind in (1, 2, 3):
            z_copy(kind, off).wait_recv()
        w_forward(off).start()
    lax.fori_loop(0, count, pool, 0)
    for off in order:
        w_forward(off).wait_recv()

    def project(b, carry):
        acc = jnp.dot(norm_all[span(b, rows), :], w_all[...], preferred_element_type=f32)
        k_all[span(b, rows), :] = acc[:, 0:LANES].astype(bf16)
        v_all[span(b, rows), :] = acc[:, LANES : 2 * LANES].astype(bf16)
        q_all[span(b, rows), :] = acc[:, 2 * LANES : 3 * LANES].astype(bf16)
        return carry

    lax.fori_loop(0, count, project, 0)

    def head_copy(b, off):
        place = heads_all.at[span(b, rows), span(s, LANES)]
        peer = lax.rem(s + off, count)
        return copy(place, place, h_send.at[b, off], h_recv.at[b, off], {"sp": peer})

    def lt_copy(b):
        return copy(lt_send.at[b], lt_in.at[s], l_send.at[b], l_recv.at[s], {"sp": b})

    lane = lax.broadcasted_iota(jnp.int32, (rows, LANES), 1)
    lt_rows = lt_send.shape[2]

    def attend(b, carry):
        q = q_all[span(b, rows), :]
        reads, logs = [], []
        for m in range(2):
            q_m = jnp.where((lane >= HD) == (m == 1), q, jnp.zeros_like(q))
            scores = (
                lax.dot_general(
                    q_m, k_all[...], (((1,), (1,)), ((), ())), preferred_element_type=f32
                )
                * HD ** (-0.5)
            )
            highest = jnp.max(scores, axis=-1, keepdims=True)
            weights = jnp.exp(scores - highest)
            totals = jnp.sum(weights, axis=-1, keepdims=True)
            reads.append(
                jnp.dot(weights.astype(bf16), v_all[...], preferred_element_type=f32) / totals
            )
            logs.append(highest + jnp.log(totals))
        contrast = reads[0] - lam[s] * reads[1]
        scaled = (
            contrast
            * lax.rsqrt(jnp.mean(contrast * contrast, axis=-1, keepdims=True) + epsilon)
            * hgain[pl.ds(s, 1), :]
        )
        heads_all[span(b, rows), span(s, LANES)] = scaled.astype(bf16)
        for off in order:
            head_copy(b, off).start()
        both = jnp.where(lane == 0, logs[0], logs[1])
        padded = jnp.concatenate([both, jnp.zeros((lt_rows - rows, LANES), f32)], axis=0)
        lt_send[b] = jnp.transpose(padded)[0:8, :]

        @pl.when(b != s)
        def _():
            lt_copy(b).start()

        return carry

    lax.fori_loop(0, count, attend, 0)

    sub = rows // 4
    peers = (sib, far, diag)

    def part_copy(b, j):
        return copy(
            part_out.at[b, peers[j]],
            part_in.at[b, j],
            p_send.at[b, j],
            p_recv.at[b, j],
            {"tp": peers[j]},
        )

    def outward(b, carry):
        for off in order:
            head_copy(b, off).wait_recv()
        total = jnp.dot(heads_all[span(b, rows), :], wao[...], preferred_element_type=f32)
        total = total + jnp.dot(
            pooled_all[span(b, rows), :], wpo[...], preferred_element_type=f32
        )
        for j in range(4):
            part_out[b, j] = total[j * sub : (j + 1) * sub, :].astype(bf16)
        for j in (2, 1, 0):
            part_copy(b, j).start()
        return carry

    lax.fori_loop(0, count, outward, 0)

    def out_copy(b):
        return copy(block_out.at[b], block_in.at[s], o_send.at[b], o_recv.at[s], {"sp": b})

    def finish(b, carry):
        total = part_out[b, t].astype(f32)
        for j in range(3):
            part_copy(b, j).wait_recv()
            total = total + part_in[b, j].astype(f32)
        block_out[b] = total.astype(bf16)

        @pl.when(b != s)
        def _():
            out_copy(b).start()

        return carry

    lax.fori_loop(0, count, finish, 0)
    for b in range(count):
        cols = slice(b * group, (b + 1) * group)

        @pl.when(s == b)
        def _():
            mixed_out[:, cols] = block_out[b]
            lt_out[b] = lt_send[b]

        @pl.when(s != b)
        def _():
            copy(
                block_out.at[s], block_in.at[b], o_send.at[s], o_recv.at[b], {"sp": b}
            ).wait_recv()
            copy(lt_send.at[s], lt_in.at[b], l_send.at[s], l_recv.at[b], {"sp": b}).wait_recv()
            mixed_out[:, cols] = block_in[b]
            lt_out[b] = lt_in[b]
            out_copy(b).wait_send()
            lt_copy(b).wait_send()

    for off in order:
        for kind in range(4):
            z_copy(kind, off).wait_send()
        for step in range(3):
            tok_forward(step, off).wait_send()
        w_forward(off).wait_send()

    def drain(b, carry):
        for off in order:
            head_copy(b, off).wait_send()
        for j in range(3):
            part_copy(b, j).wait_send()
        return carry

    lax.fori_loop(0, count, drain, 0)


def fused(
    count,
    tokens,
    norm_gain,
    query_weight,
    key_weight,
    value_weight,
    map_lambda,
    head_gain,
    attn_out_weight,
    pool_out_weight,
):
    rows, width = tokens.shape
    cols = attn_out_weight.shape[1]
    sub = rows // 4
    seq = rows * count
    lt_rows = -(-rows // LANES) * LANES
    bf16, f32 = jnp.bfloat16, jnp.float32
    vmem = pl.BlockSpec(memory_space=pltpu.VMEM)
    smem = pl.BlockSpec(memory_space=pltpu.SMEM)
    sems = pltpu.SemaphoreType.DMA
    mixed, logs = pl.pallas_call(
        functools.partial(fused_kernel, count),
        out_shape=(
            jax.ShapeDtypeStruct((sub, width), bf16),
            jax.ShapeDtypeStruct((count, 8, lt_rows), f32),
        ),
        in_specs=[vmem] * 5 + [smem] + [vmem] * 3,
        out_specs=(vmem, vmem),
        scratch_shapes=[
            pltpu.VMEM((seq, width), bf16),
            pltpu.VMEM((seq, width), bf16),
            pltpu.VMEM((width, 3 * LANES), bf16),
            pltpu.VMEM((seq, LANES), bf16),
            pltpu.VMEM((seq, LANES), bf16),
            pltpu.VMEM((seq, LANES), bf16),
            pltpu.VMEM((seq, count * LANES), bf16),
            pltpu.VMEM((seq, pool_out_weight.shape[0]), bf16),
            pltpu.VMEM((count, 4, sub, cols), bf16),
            pltpu.VMEM((count, 3, sub, cols), bf16),
            pltpu.VMEM((count, sub, cols), bf16),
            pltpu.VMEM((count, sub, cols), bf16),
            pltpu.VMEM((count, 8, lt_rows), f32),
            pltpu.VMEM((count, 8, lt_rows), f32),
            sems((4, count)),
            sems((4, count)),
            sems((4, count)),
            sems((4, count)),
            sems((count, count)),
            sems((count, count)),
            sems((count, 3)),
            sems((count, 3)),
            sems((count,)),
            sems((count,)),
            sems((count,)),
            sems((count,)),
        ],
        compiler_params=pltpu.CompilerParams(collective_id=0, has_side_effects=True),
    )(
        tokens,
        norm_gain.reshape(1, width),
        query_weight,
        key_weight,
        value_weight,
        map_lambda,
        head_gain,
        attn_out_weight,
        pool_out_weight,
    )
    return mixed, jnp.transpose(logs[:, 0:2, 0:rows], (1, 0, 2))


def fits(shape, tokens, query_weight, value_weight, map_lambda, pool_out_weight):
    count = shape["sp"]
    return (
        shape["grp"] == 2
        and shape["tp"] == 4
        and count > 1
        and map_lambda.shape[0] == count
        and value_weight.shape[1] == VD == LANES == 2 * HD
        and tokens.shape[0] % 32 == 0
        and tokens.shape[1] % (4 * LANES) == 0
        and query_weight.shape[0] % 32 == 0
        and pool_out_weight.shape[0] * 4 == tokens.shape[1]
        and pool_out_weight.shape[1] % LANES == 0
        and pool_out_weight.shape[1] * count == tokens.shape[1]
        and pool_out_weight.shape[0] == pool_out_weight.shape[1]
        and tokens.shape[0] * count * tokens.shape[1] <= 1 << 22
    )


def solution(mesh):
    placed = (
        P(("grp", "sp"), None),
        P(),
        P("sp", "tp"),
        P("sp", "tp"),
        P("sp", "tp"),
        P("tp"),
        P("tp", None),
        P("tp", "sp"),
        P("tp", "sp"),
    )
    shape = dict(mesh.shape)

    def chosen(*args):
        if fits(shape, args[0], args[2], args[4], args[5], args[8]):
            return fused(shape["sp"], *args)
        return on_device(*args)

    return jax.shard_map(
        chosen,
        mesh=mesh,
        in_specs=placed,
        out_specs=(P(("grp", "sp", "tp"), None), P(None, "tp", ("grp", "sp"))),
        check_vma=False,
    )
```

```python
import functools
import math

import jax
import jax.numpy as jnp
from jax import lax
from jax.experimental import pallas as pl
from jax.experimental.pallas import tpu as pltpu
from jax.sharding import PartitionSpec as P

HD = 64
VD = 128
POOL_SPAN = 16


epsilon = 1e-06
very_low = -1e30


def extended(cells, sides, width):
    for axis, dim in sides:
        count = lax.axis_size(axis)
        ends = count - 1
        head = lax.slice_in_dim(cells, 0, width, axis=dim)
        tail = lax.slice_in_dim(cells, cells.shape[dim] - width, cells.shape[dim], axis=dim)
        cells = jnp.concatenate(
            [
                lax.ppermute(tail, axis, [(i, (i + 1) % count) for i in range(ends)]),
                cells,
                lax.ppermute(head, axis, [((i + 1) % count, i) for i in range(ends)]),
            ],
            axis=dim,
        )
    return cells


def add_products(totals, pieces, source):
    results = []
    for running, piece in zip(totals, pieces):
        results.append(jnp.dot(source, piece, preferred_element_type=jnp.float32))
    return tuple(results)


def on_device(
    tokens,
    norm_gain,
    query_weight,
    key_weight,
    value_weight,
    map_lambda,
    head_gain,
    attn_out_weight,
    pool_out_weight,
):
    tokens_wide = tokens.astype(jnp.float32)
    normed = (
        tokens_wide
        * lax.rsqrt(jnp.mean(tokens_wide * tokens_wide, axis=-1, keepdims=True) + epsilon)
        * norm_gain
    ).astype(jnp.bfloat16)
    row_count = normed.shape[0]
    sp_index = lax.axis_index("sp")
    tp_index = lax.axis_index("tp")
    group_width = pool_out_weight.shape[0]
    local_heads = map_lambda.shape[0]
    key_heads = value_weight.shape[1] // VD
    group_heads = local_heads // key_heads
    q_empty = jnp.zeros((row_count, query_weight.shape[1]), jnp.float32)
    k_empty = jnp.zeros((row_count, key_weight.shape[1]), jnp.float32)
    v_empty = jnp.zeros((row_count, value_weight.shape[1]), jnp.float32)
    q_acc, k_acc, v_acc = add_products(
        (q_empty, k_empty, v_empty),
        (
            lax.all_gather(query_weight, "sp", axis=0, tiled=True),
            lax.all_gather(key_weight, "sp", axis=0, tiled=True),
            lax.all_gather(value_weight, "sp", axis=0, tiled=True),
        ),
        normed,
    )
    queries = q_acc.astype(jnp.bfloat16).reshape(row_count, key_heads, group_heads, 2, HD)
    keys_flat = k_acc.astype(jnp.bfloat16)
    values_flat = v_acc.astype(jnp.bfloat16)

    def key_block(state_now, key_pair):
        maxima, totals, accums = state_now
        key_blk, val_blk = key_pair
        scores = jnp.einsum(
            "qhgmd,khmd->hgmqk", queries, key_blk, preferred_element_type=jnp.float32
        ) * HD ** (-0.5)
        highest = jnp.maximum(maxima, jnp.max(scores, axis=-1))
        factor = jnp.exp(maxima - highest)
        weights = jnp.exp(scores - highest[..., None])
        totals = totals * factor + jnp.sum(weights, axis=-1)
        accums = accums * factor[..., None] + jnp.einsum(
            "hgmqk,khe->hgmqe",
            weights.astype(jnp.bfloat16),
            val_blk,
            preferred_element_type=jnp.float32,
        )
        return ((highest, totals, accums), None)

    start_state = (
        jnp.full((key_heads, group_heads, 2, row_count), very_low, jnp.float32),
        jnp.zeros((key_heads, group_heads, 2, row_count), jnp.float32),
        jnp.zeros((key_heads, group_heads, 2, row_count, VD), jnp.float32),
    )
    key_piece = lax.all_gather(keys_flat, "sp", axis=0, tiled=True)
    val_piece = lax.all_gather(values_flat, "sp", axis=0, tiled=True)
    piece_len = key_piece.shape[0]
    block_len = math.gcd(piece_len, 512)
    key_blocks = key_piece.reshape(piece_len // block_len, block_len, key_heads, 2, HD)
    val_blocks = val_piece.reshape(piece_len // block_len, block_len, key_heads, VD)
    state_next, unused = lax.scan(key_block, start_state, (key_blocks, val_blocks))
    maxima, totals, accums = state_next
    log_parts = maxima + jnp.log(totals)
    log_totals = jnp.transpose(log_parts, (2, 0, 1, 3)).reshape(2, local_heads, row_count)
    reads = accums / totals[..., None]
    contrast = reads[:, :, 0] - map_lambda.reshape(key_heads, group_heads, 1, 1) * reads[:, :, 1]
    scaled = (
        contrast
        * lax.rsqrt(jnp.mean(contrast * contrast, axis=-1, keepdims=True) + epsilon)
        * head_gain.reshape(key_heads, group_heads, 1, VD)
    )
    attention_head_rows = (
        jnp.transpose(scaled, (2, 0, 1, 3))
        .reshape(row_count, local_heads * VD)
        .astype(jnp.bfloat16)
    )
    head_rows, log_totals = (attention_head_rows, log_totals)
    own_chan = lax.dynamic_slice_in_dim(normed, tp_index * group_width, group_width, 1)
    reach = POOL_SPAN // 2
    padded = extended(own_chan, (("sp", 0),), reach)
    window = jnp.left_shift(jnp.int32(2), tp_index)
    half_span = window // 2
    running = jnp.zeros((row_count, group_width), jnp.float32)
    for offset in range(POOL_SPAN):
        piece = lax.dynamic_slice_in_dim(padded, reach - half_span + offset, row_count, 0).astype(
            jnp.float32
        )
        running = running + jnp.where(offset < window, piece, 0.0)
    seq_len = row_count * lax.axis_size("sp")
    position = sp_index * row_count + jnp.arange(row_count, dtype=jnp.int32)
    lower_edge = jnp.clip(position - half_span, 0, seq_len)
    upper_edge = jnp.clip(position + window - half_span, 0, seq_len)
    counts_f = (upper_edge - lower_edge).astype(jnp.float32)[:, None]
    pooled = (running / counts_f - own_chan.astype(jnp.float32)).astype(jnp.bfloat16)
    attn_whole, pool_whole = (
        lax.all_gather(attn_out_weight, "sp", axis=1, tiled=True),
        lax.all_gather(pool_out_weight, "sp", axis=1, tiled=True),
    )
    mixed = lax.psum_scatter(
        (
            jnp.dot(head_rows, attn_whole, preferred_element_type=jnp.float32)
            + jnp.dot(pooled, pool_whole, preferred_element_type=jnp.float32)
        ).astype(jnp.bfloat16),
        "tp",
        scatter_dimension=0,
        tiled=True,
    )
    return (mixed, log_totals)


MESH = pl.DeviceIdType.MESH
LANES = 128


def fused_kernel(
    count,
    tok,
    gain,
    wq,
    wk,
    wv,
    lam,
    hgain,
    wao,
    wpo,
    mixed_out,
    lt_out,
    tok_all,
    norm_all,
    w_all,
    q_all,
    k_all,
    v_all,
    heads_all,
    pooled_all,
    part_out,
    part_in,
    block_out,
    block_in,
    lt_send,
    lt_in,
    wao_in,
    wpo_in,
    local_sem,
    q_send,
    q_recv,
    z_send,
    z_recv,
    f_send,
    f_recv,
    h_send,
    h_recv,
    p_send,
    p_recv,
    o_send,
    o_recv,
    l_send,
    l_recv,
):
    g = lax.axis_index("grp")
    s = lax.axis_index("sp")
    t = lax.axis_index("tp")
    rows, width = tok.shape
    quarter = width // 4
    shard = wq.shape[0]
    half = shard // 2
    sib = t + 1 - 2 * lax.rem(t, 2)
    far = lax.rem(t + 2, 4)
    diag = lax.rem(sib + 2, 4)
    twin = 1 - g
    offs = list(range(1, count))
    order = sorted(offs, key=lambda o: min(o, count - o))
    f32, bf16 = jnp.float32, jnp.bfloat16

    def span(index, size):
        return pl.ds(pl.multiple_of(index * size, size), size)

    def half_rows(owner, part):
        return pl.ds(pl.multiple_of(owner * shard + part * half, half), half)

    pieces = (
        (tok, tok_all.at[span(s, rows), :]),
        (wk, w_all.at[span(s, shard), 0:LANES]),
        (wv, w_all.at[span(s, shard), LANES : 2 * LANES]),
        (wq.at[:, span(s, LANES)], w_all.at[span(s, shard), 2 * LANES : 3 * LANES]),
        (wao, wao_in),
        (wpo, wpo_in),
    )
    local = [
        pltpu.make_async_copy(src, dst, local_sem.at[i]) for i, (src, dst) in enumerate(pieces)
    ]
    for piece in local:
        piece.start()
    barrier = pltpu.get_barrier_semaphore()
    for off in offs:
        pl.semaphore_signal(
            barrier, inc=1, device_id={"sp": lax.rem(s + off, count)}, device_id_type=MESH
        )
    for peer in (sib, far, diag):
        pl.semaphore_signal(barrier, inc=1, device_id={"tp": peer}, device_id_type=MESH)
    pl.semaphore_signal(barrier, inc=1, device_id={"grp": twin}, device_id_type=MESH)
    pl.semaphore_wait(barrier, count - 1 + 4)

    def copy(src, dst, send, recv, where):
        return pltpu.make_async_remote_copy(
            src_ref=src,
            dst_ref=dst,
            send_sem=send,
            recv_sem=recv,
            device_id=where,
            device_id_type=MESH,
        )

    kv = slice(0, 2 * LANES)
    qs = slice(2 * LANES, 3 * LANES)

    def z_copy(kind, owner, up):
        if kind == 0:
            place = tok_all.at[span(owner, rows), span(t, quarter)]
        else:
            place = w_all.at[half_rows(owner, g), kv]
        step = 1 if up else -1
        return copy(
            place,
            place,
            z_send.at[kind, owner, int(up)],
            z_recv.at[kind, owner],
            {"sp": lax.rem(s + step + count, count)},
        )

    def q_copy(off):
        peer = lax.rem(s + off, count)
        src = wq.at[span(g, half), span(peer, LANES)]
        dst = w_all.at[half_rows(s, g), qs]
        return copy(src, dst, q_send.at[off], q_recv.at[s], {"sp": peer})

    def q_arrival(owner):
        place = w_all.at[half_rows(owner, g), qs]
        return copy(place, place, q_send.at[0], q_recv.at[owner], {"sp": owner})

    def tok_forward(step, owner):
        col = span(far if step == 2 else t, quarter)
        place = tok_all.at[span(owner, rows), col]
        where = {"tp": far if step == 1 else sib}
        return copy(place, place, f_send.at[step, owner], f_recv.at[step, owner], where)

    def w_forward(kind, owner):
        place = w_all.at[half_rows(owner, g), qs if kind else kv]
        at = 3 + kind
        return copy(place, place, f_send.at[at, owner], f_recv.at[at, owner], {"grp": twin})

    def sides(k, act):
        @pl.when(s >= k)
        def _():
            act(s - k, True, s < count - 1)

        @pl.when(s + k < count)
        def _():
            act(s + k, False, s > 0)

    def both_ways(act):
        @pl.when(s < count - 1)
        def _():
            act(True)

        @pl.when(s > 0)
        def _():
            act(False)

    local[0].wait()
    both_ways(lambda up: z_copy(0, s, up).start())
    local[1].wait()
    local[2].wait()
    both_ways(lambda up: z_copy(1, s, up).start())
    for off in order:
        q_copy(off).start()

    def norm_block(owner):
        step = 16

        def one(i, carry):
            at = pl.ds(pl.multiple_of(owner * rows + i * step, step), step)
            x = tok_all[at, :].astype(f32)
            scale = lax.rsqrt(jnp.mean(x * x, axis=-1, keepdims=True) + epsilon)
            norm_all[at, :] = (x * scale * gain[...]).astype(bf16)
            return carry

        lax.fori_loop(0, rows // step, one, 0)

    def z_tok(owner, up, more):
        z_copy(0, owner, True).wait_recv()

        @pl.when(more)
        def _():
            z_copy(0, owner, up).start()

        tok_forward(1, owner).start()
        tok_forward(0, owner).start()

    def z_weight(owner, up, more):
        z_copy(1, owner, True).wait_recv()

        @pl.when(more)
        def _():
            z_copy(1, owner, up).start()

        w_forward(0, owner).start()
        q_arrival(owner).wait_recv()
        w_forward(1, owner).start()

    def x_tok(owner, up, more):
        tok_forward(1, owner).wait_recv()
        tok_forward(2, owner).start()

    def norm_owner(owner, up, more):
        tok_forward(0, owner).wait_recv()
        tok_forward(2, owner).wait_recv()
        norm_block(owner)

    norm_block(s)
    last = count - 1
    for k in range(1, count):
        sides(k, z_tok)
        if k > 1:
            sides(k - 1, x_tok)
        if k > 2:
            sides(k - 2, norm_owner)
        sides(k, z_weight)
    if last > 1:
        sides(last - 1, norm_owner)
    sides(last, x_tok)
    sides(last, norm_owner)

    seq = rows * count
    group = wpo.shape[0]
    window = jnp.where(t == 0, 2, jnp.where(t == 1, 4, jnp.where(t == 2, 8, 16)))
    half_span = window // 2

    def pool(b, carry):
        at = b * rows + lax.broadcasted_iota(jnp.int32, (rows, seq), 0)
        col = lax.broadcasted_iota(jnp.int32, (rows, seq), 1)
        inside = (col >= at - half_span) & (col < at + window - half_span)
        band = jnp.where(inside, 1.0, 0.0).astype(bf16)
        total = jnp.dot(band, norm_all[:, span(t, group)], preferred_element_type=f32)
        pos = b * rows + lax.broadcasted_iota(jnp.int32, (rows, 1), 0)
        low = jnp.maximum(pos - half_span, 0)
        high = jnp.minimum(pos + window - half_span, seq)
        own = norm_all[span(b, rows), span(t, group)].astype(f32)
        pooled_all[span(b, rows), :] = (total / (high - low).astype(f32) - own).astype(bf16)
        return carry

    lax.fori_loop(0, count, pool, 0)

    def y_arrival(owner, up, more):
        w_forward(0, owner).wait_recv()
        w_forward(1, owner).wait_recv()

    for k in range(1, count):
        sides(k, y_arrival)
    local[3].wait()

    def project(b, carry):
        acc = jnp.dot(norm_all[span(b, rows), :], w_all[...], preferred_element_type=f32)
        k_all[span(b, rows), :] = acc[:, 0:LANES].astype(bf16)
        v_all[span(b, rows), :] = acc[:, LANES : 2 * LANES].astype(bf16)
        q_all[span(b, rows), :] = acc[:, 2 * LANES : 3 * LANES].astype(bf16)
        return carry

    lax.fori_loop(0, count, project, 0)

    def head_copy(b, off):
        place = heads_all.at[span(b, rows), span(s, LANES)]
        peer = lax.rem(s + off, count)
        return copy(place, place, h_send.at[b, off], h_recv.at[b, off], {"sp": peer})

    def lt_copy(b):
        return copy(lt_send.at[b], lt_in.at[s], l_send.at[b], l_recv.at[s], {"sp": b})

    lane = lax.broadcasted_iota(jnp.int32, (rows, LANES), 1)
    lt_rows = lt_send.shape[2]

    def attend(b, carry):
        q = q_all[span(b, rows), :]
        reads, logs = [], []
        for m in range(2):
            q_m = jnp.where((lane >= HD) == (m == 1), q, jnp.zeros_like(q))
            scores = (
                lax.dot_general(
                    q_m, k_all[...], (((1,), (1,)), ((), ())), preferred_element_type=f32
                )
                * HD ** (-0.5)
            )
            highest = jnp.max(scores, axis=-1, keepdims=True)
            weights = jnp.exp(scores - highest)
            totals = jnp.sum(weights, axis=-1, keepdims=True)
            reads.append(
                jnp.dot(weights.astype(bf16), v_all[...], preferred_element_type=f32) / totals
            )
            logs.append(highest + jnp.log(totals))
        contrast = reads[0] - lam[s] * reads[1]
        scaled = (
            contrast
            * lax.rsqrt(jnp.mean(contrast * contrast, axis=-1, keepdims=True) + epsilon)
            * hgain[pl.ds(s, 1), :]
        )
        heads_all[span(b, rows), span(s, LANES)] = scaled.astype(bf16)
        for off in order:
            head_copy(b, off).start()
        both = jnp.where(lane == 0, logs[0], logs[1])
        padded = jnp.concatenate([both, jnp.zeros((lt_rows - rows, LANES), f32)], axis=0)
        lt_send[b] = jnp.transpose(padded)[0:8, :]

        @pl.when(b != s)
        def _():
            lt_copy(b).start()

        return carry

    lax.fori_loop(0, count, attend, 0)

    sub = rows // 4
    peers = (sib, far, diag)

    def part_copy(b, j):
        return copy(
            part_out.at[b, peers[j]],
            part_in.at[b, j],
            p_send.at[b, j],
            p_recv.at[b, j],
            {"tp": peers[j]},
        )

    local[4].wait()
    local[5].wait()

    def outward(b, carry):
        for off in order:
            head_copy(b, off).wait_recv()
        total = jnp.dot(heads_all[span(b, rows), :], wao_in[...], preferred_element_type=f32)
        total = total + jnp.dot(
            pooled_all[span(b, rows), :], wpo_in[...], preferred_element_type=f32
        )
        for j in range(4):
            part_out[b, j] = total[j * sub : (j + 1) * sub, :].astype(bf16)
        for j in (2, 1, 0):
            part_copy(b, j).start()
        return carry

    lax.fori_loop(0, count, outward, 0)

    def out_copy(b):
        return copy(block_out.at[b], block_in.at[s], o_send.at[b], o_recv.at[s], {"sp": b})

    def finish(b, carry):
        total = part_out[b, t].astype(f32)
        for j in range(3):
            part_copy(b, j).wait_recv()
            total = total + part_in[b, j].astype(f32)
        block_out[b] = total.astype(bf16)

        @pl.when(b != s)
        def _():
            out_copy(b).start()

        return carry

    lax.fori_loop(0, count, finish, 0)
    for b in range(count):
        cols = slice(b * group, (b + 1) * group)

        @pl.when(s == b)
        def _():
            mixed_out[:, cols] = block_out[b]
            lt_out[b] = lt_send[b]

        @pl.when(s != b)
        def _():
            copy(
                block_out.at[s], block_in.at[b], o_send.at[s], o_recv.at[b], {"sp": b}
            ).wait_recv()
            copy(lt_send.at[s], lt_in.at[b], l_send.at[s], l_recv.at[b], {"sp": b}).wait_recv()
            mixed_out[:, cols] = block_in[b]
            lt_out[b] = lt_in[b]
            out_copy(b).wait_send()
            lt_copy(b).wait_send()

    both_ways(lambda up: z_copy(0, s, up).wait_send())
    both_ways(lambda up: z_copy(1, s, up).wait_send())
    for off in order:
        q_copy(off).wait_send()

    def sent(owner, up, more):
        @pl.when(more)
        def _():
            z_copy(0, owner, up).wait_send()
            z_copy(1, owner, up).wait_send()

        for step in range(3):
            tok_forward(step, owner).wait_send()
        w_forward(0, owner).wait_send()
        w_forward(1, owner).wait_send()

    for k in range(1, count):
        sides(k, sent)

    def drain(b, carry):
        for off in order:
            head_copy(b, off).wait_send()
        for j in range(3):
            part_copy(b, j).wait_send()
        return carry

    lax.fori_loop(0, count, drain, 0)


def fused(
    count,
    tokens,
    norm_gain,
    query_weight,
    key_weight,
    value_weight,
    map_lambda,
    head_gain,
    attn_out_weight,
    pool_out_weight,
):
    rows, width = tokens.shape
    cols = attn_out_weight.shape[1]
    sub = rows // 4
    seq = rows * count
    lt_rows = -(-rows // LANES) * LANES
    bf16, f32 = jnp.bfloat16, jnp.float32
    vmem = pl.BlockSpec(memory_space=pltpu.VMEM)
    smem = pl.BlockSpec(memory_space=pltpu.SMEM)
    far = pl.BlockSpec(memory_space=pl.ANY)
    sems = pltpu.SemaphoreType.DMA
    mixed, logs = pl.pallas_call(
        functools.partial(fused_kernel, count),
        out_shape=(
            jax.ShapeDtypeStruct((sub, width), bf16),
            jax.ShapeDtypeStruct((count, 8, lt_rows), f32),
        ),
        in_specs=[far, vmem, far, far, far, smem, vmem, far, far],
        out_specs=(vmem, vmem),
        scratch_shapes=[
            pltpu.VMEM((seq, width), bf16),
            pltpu.VMEM((seq, width), bf16),
            pltpu.VMEM((width, 3 * LANES), bf16),
            pltpu.VMEM((seq, LANES), bf16),
            pltpu.VMEM((seq, LANES), bf16),
            pltpu.VMEM((seq, LANES), bf16),
            pltpu.VMEM((seq, count * LANES), bf16),
            pltpu.VMEM((seq, pool_out_weight.shape[0]), bf16),
            pltpu.VMEM((count, 4, sub, cols), bf16),
            pltpu.VMEM((count, 3, sub, cols), bf16),
            pltpu.VMEM((count, sub, cols), bf16),
            pltpu.VMEM((count, sub, cols), bf16),
            pltpu.VMEM((count, 8, lt_rows), f32),
            pltpu.VMEM((count, 8, lt_rows), f32),
            pltpu.VMEM(attn_out_weight.shape, bf16),
            pltpu.VMEM(pool_out_weight.shape, bf16),
            sems((6,)),
            sems((count,)),
            sems((count,)),
            sems((2, count, 2)),
            sems((2, count)),
            sems((5, count)),
            sems((5, count)),
            sems((count, count)),
            sems((count, count)),
            sems((count, 3)),
            sems((count, 3)),
            sems((count,)),
            sems((count,)),
            sems((count,)),
            sems((count,)),
        ],
        compiler_params=pltpu.CompilerParams(collective_id=0, has_side_effects=True),
    )(
        tokens,
        norm_gain.reshape(1, width),
        query_weight,
        key_weight,
        value_weight,
        map_lambda,
        head_gain,
        attn_out_weight,
        pool_out_weight,
    )
    return mixed, jnp.transpose(logs[:, 0:2, 0:rows], (1, 0, 2))


def fits(shape, tokens, query_weight, value_weight, map_lambda, pool_out_weight):
    count = shape["sp"]
    return (
        shape["grp"] == 2
        and shape["tp"] == 4
        and count > 1
        and map_lambda.shape[0] == count
        and value_weight.shape[1] == VD == LANES == 2 * HD
        and tokens.shape[0] % 32 == 0
        and tokens.shape[1] % (4 * LANES) == 0
        and query_weight.shape[0] % 32 == 0
        and pool_out_weight.shape[0] * 4 == tokens.shape[1]
        and pool_out_weight.shape[1] % LANES == 0
        and pool_out_weight.shape[1] * count == tokens.shape[1]
        and pool_out_weight.shape[0] == pool_out_weight.shape[1]
        and tokens.shape[0] * count * tokens.shape[1] <= 1 << 22
    )


def solution(mesh):
    placed = (
        P(("grp", "sp"), None),
        P(),
        P("sp", "tp"),
        P("sp", "tp"),
        P("sp", "tp"),
        P("tp"),
        P("tp", None),
        P("tp", "sp"),
        P("tp", "sp"),
    )
    shape = dict(mesh.shape)

    def chosen(*args):
        if fits(shape, args[0], args[2], args[4], args[5], args[8]):
            return fused(shape["sp"], *args)
        return on_device(*args)

    return jax.shard_map(
        chosen,
        mesh=mesh,
        in_specs=placed,
        out_specs=(P(("grp", "sp", "tp"), None), P(None, "tp", ("grp", "sp"))),
        check_vma=False,
    )
```

```python
import functools
import math

import jax
import jax.numpy as jnp
from jax import lax
from jax.experimental import pallas as pl
from jax.experimental.pallas import tpu as pltpu
from jax.sharding import PartitionSpec as P

HD = 64
VD = 128
POOL_SPAN = 16


epsilon = 1e-06
very_low = -1e30


def extended(cells, sides, width):
    for axis, dim in sides:
        count = lax.axis_size(axis)
        ends = count - 1
        head = lax.slice_in_dim(cells, 0, width, axis=dim)
        tail = lax.slice_in_dim(cells, cells.shape[dim] - width, cells.shape[dim], axis=dim)
        cells = jnp.concatenate(
            [
                lax.ppermute(tail, axis, [(i, (i + 1) % count) for i in range(ends)]),
                cells,
                lax.ppermute(head, axis, [((i + 1) % count, i) for i in range(ends)]),
            ],
            axis=dim,
        )
    return cells


def add_products(totals, pieces, source):
    results = []
    for running, piece in zip(totals, pieces):
        results.append(jnp.dot(source, piece, preferred_element_type=jnp.float32))
    return tuple(results)


def on_device(
    tokens,
    norm_gain,
    query_weight,
    key_weight,
    value_weight,
    map_lambda,
    head_gain,
    attn_out_weight,
    pool_out_weight,
):
    tokens_wide = tokens.astype(jnp.float32)
    normed = (
        tokens_wide
        * lax.rsqrt(jnp.mean(tokens_wide * tokens_wide, axis=-1, keepdims=True) + epsilon)
        * norm_gain
    ).astype(jnp.bfloat16)
    row_count = normed.shape[0]
    sp_index = lax.axis_index("sp")
    tp_index = lax.axis_index("tp")
    group_width = pool_out_weight.shape[0]
    local_heads = map_lambda.shape[0]
    key_heads = value_weight.shape[1] // VD
    group_heads = local_heads // key_heads
    q_empty = jnp.zeros((row_count, query_weight.shape[1]), jnp.float32)
    k_empty = jnp.zeros((row_count, key_weight.shape[1]), jnp.float32)
    v_empty = jnp.zeros((row_count, value_weight.shape[1]), jnp.float32)
    q_acc, k_acc, v_acc = add_products(
        (q_empty, k_empty, v_empty),
        (
            lax.all_gather(query_weight, "sp", axis=0, tiled=True),
            lax.all_gather(key_weight, "sp", axis=0, tiled=True),
            lax.all_gather(value_weight, "sp", axis=0, tiled=True),
        ),
        normed,
    )
    queries = q_acc.astype(jnp.bfloat16).reshape(row_count, key_heads, group_heads, 2, HD)
    keys_flat = k_acc.astype(jnp.bfloat16)
    values_flat = v_acc.astype(jnp.bfloat16)

    def key_block(state_now, key_pair):
        maxima, totals, accums = state_now
        key_blk, val_blk = key_pair
        scores = jnp.einsum(
            "qhgmd,khmd->hgmqk", queries, key_blk, preferred_element_type=jnp.float32
        ) * HD ** (-0.5)
        highest = jnp.maximum(maxima, jnp.max(scores, axis=-1))
        factor = jnp.exp(maxima - highest)
        weights = jnp.exp(scores - highest[..., None])
        totals = totals * factor + jnp.sum(weights, axis=-1)
        accums = accums * factor[..., None] + jnp.einsum(
            "hgmqk,khe->hgmqe",
            weights.astype(jnp.bfloat16),
            val_blk,
            preferred_element_type=jnp.float32,
        )
        return ((highest, totals, accums), None)

    start_state = (
        jnp.full((key_heads, group_heads, 2, row_count), very_low, jnp.float32),
        jnp.zeros((key_heads, group_heads, 2, row_count), jnp.float32),
        jnp.zeros((key_heads, group_heads, 2, row_count, VD), jnp.float32),
    )
    key_piece = lax.all_gather(keys_flat, "sp", axis=0, tiled=True)
    val_piece = lax.all_gather(values_flat, "sp", axis=0, tiled=True)
    piece_len = key_piece.shape[0]
    block_len = math.gcd(piece_len, 512)
    key_blocks = key_piece.reshape(piece_len // block_len, block_len, key_heads, 2, HD)
    val_blocks = val_piece.reshape(piece_len // block_len, block_len, key_heads, VD)
    state_next, unused = lax.scan(key_block, start_state, (key_blocks, val_blocks))
    maxima, totals, accums = state_next
    log_parts = maxima + jnp.log(totals)
    log_totals = jnp.transpose(log_parts, (2, 0, 1, 3)).reshape(2, local_heads, row_count)
    reads = accums / totals[..., None]
    contrast = reads[:, :, 0] - map_lambda.reshape(key_heads, group_heads, 1, 1) * reads[:, :, 1]
    scaled = (
        contrast
        * lax.rsqrt(jnp.mean(contrast * contrast, axis=-1, keepdims=True) + epsilon)
        * head_gain.reshape(key_heads, group_heads, 1, VD)
    )
    attention_head_rows = (
        jnp.transpose(scaled, (2, 0, 1, 3))
        .reshape(row_count, local_heads * VD)
        .astype(jnp.bfloat16)
    )
    head_rows, log_totals = (attention_head_rows, log_totals)
    own_chan = lax.dynamic_slice_in_dim(normed, tp_index * group_width, group_width, 1)
    reach = POOL_SPAN // 2
    padded = extended(own_chan, (("sp", 0),), reach)
    window = jnp.left_shift(jnp.int32(2), tp_index)
    half_span = window // 2
    running = jnp.zeros((row_count, group_width), jnp.float32)
    for offset in range(POOL_SPAN):
        piece = lax.dynamic_slice_in_dim(padded, reach - half_span + offset, row_count, 0).astype(
            jnp.float32
        )
        running = running + jnp.where(offset < window, piece, 0.0)
    seq_len = row_count * lax.axis_size("sp")
    position = sp_index * row_count + jnp.arange(row_count, dtype=jnp.int32)
    lower_edge = jnp.clip(position - half_span, 0, seq_len)
    upper_edge = jnp.clip(position + window - half_span, 0, seq_len)
    counts_f = (upper_edge - lower_edge).astype(jnp.float32)[:, None]
    pooled = (running / counts_f - own_chan.astype(jnp.float32)).astype(jnp.bfloat16)
    attn_whole, pool_whole = (
        lax.all_gather(attn_out_weight, "sp", axis=1, tiled=True),
        lax.all_gather(pool_out_weight, "sp", axis=1, tiled=True),
    )
    mixed = lax.psum_scatter(
        (
            jnp.dot(head_rows, attn_whole, preferred_element_type=jnp.float32)
            + jnp.dot(pooled, pool_whole, preferred_element_type=jnp.float32)
        ).astype(jnp.bfloat16),
        "tp",
        scatter_dimension=0,
        tiled=True,
    )
    return (mixed, log_totals)


MESH = pl.DeviceIdType.MESH
LANES = 128


def fused_kernel(
    count,
    tok,
    gain,
    wq,
    wk,
    wv,
    lam,
    hgain,
    wao,
    wpo,
    mixed_out,
    lt_out,
    tok_all,
    norm_all,
    w_all,
    q_all,
    k_all,
    v_all,
    heads_all,
    pooled_all,
    part_out,
    part_in,
    block_out,
    block_in,
    lt_send,
    lt_in,
    wao_in,
    wpo_in,
    local_sem,
    q_send,
    q_recv,
    z_send,
    z_recv,
    f_send,
    f_recv,
    h_send,
    h_recv,
    p_send,
    p_recv,
    o_send,
    o_recv,
    l_send,
    l_recv,
):
    g = lax.axis_index("grp")
    s = lax.axis_index("sp")
    t = lax.axis_index("tp")
    rows, width = tok.shape
    quarter = width // 4
    shard = wq.shape[0]
    half = shard // 2
    sib = t + 1 - 2 * lax.rem(t, 2)
    far = lax.rem(t + 2, 4)
    diag = lax.rem(sib + 2, 4)
    twin = 1 - g
    offs = list(range(1, count))
    order = sorted(offs, key=lambda o: min(o, count - o))
    f32, bf16 = jnp.float32, jnp.bfloat16

    def span(index, size):
        return pl.ds(pl.multiple_of(index * size, size), size)

    def half_rows(owner, part):
        return pl.ds(pl.multiple_of(owner * shard + part * half, half), half)

    pieces = (
        (tok, tok_all.at[span(s, rows), :]),
        (wk, w_all.at[span(s, shard), 0:LANES]),
        (wv, w_all.at[span(s, shard), LANES : 2 * LANES]),
        (wq.at[:, span(s, LANES)], w_all.at[span(s, shard), 2 * LANES : 3 * LANES]),
        (wao, wao_in),
        (wpo, wpo_in),
    )
    local = [
        pltpu.make_async_copy(src, dst, local_sem.at[i]) for i, (src, dst) in enumerate(pieces)
    ]
    for piece in local:
        piece.start()
    barrier = pltpu.get_barrier_semaphore()
    for off in offs:
        pl.semaphore_signal(
            barrier, inc=1, device_id={"sp": lax.rem(s + off, count)}, device_id_type=MESH
        )
    for peer in (sib, far, diag):
        pl.semaphore_signal(barrier, inc=1, device_id={"tp": peer}, device_id_type=MESH)
    pl.semaphore_signal(barrier, inc=1, device_id={"grp": twin}, device_id_type=MESH)
    pl.semaphore_wait(barrier, count - 1 + 4)

    def copy(src, dst, send, recv, where):
        return pltpu.make_async_remote_copy(
            src_ref=src,
            dst_ref=dst,
            send_sem=send,
            recv_sem=recv,
            device_id=where,
            device_id_type=MESH,
        )

    kv = slice(0, 2 * LANES)
    qs = slice(2 * LANES, 3 * LANES)

    def z_copy(kind, owner, up):
        if kind == 0:
            place = tok_all.at[span(owner, rows), span(t, quarter)]
        else:
            place = w_all.at[half_rows(owner, g), kv]
        step = 1 if up else -1
        return copy(
            place,
            place,
            z_send.at[kind, owner, int(up)],
            z_recv.at[kind, owner],
            {"sp": lax.rem(s + step + count, count)},
        )

    def q_copy(off):
        peer = lax.rem(s + off, count)
        src = wq.at[span(g, half), span(peer, LANES)]
        dst = w_all.at[half_rows(s, g), qs]
        return copy(src, dst, q_send.at[off], q_recv.at[s], {"sp": peer})

    def q_arrival(owner):
        place = w_all.at[half_rows(owner, g), qs]
        return copy(place, place, q_send.at[0], q_recv.at[owner], {"sp": owner})

    def tok_forward(step, owner):
        col = span(far if step == 2 else t, quarter)
        place = tok_all.at[span(owner, rows), col]
        where = {"tp": far if step == 1 else sib}
        return copy(place, place, f_send.at[step, owner], f_recv.at[step, owner], where)

    def w_forward(kind, owner):
        place = w_all.at[half_rows(owner, g), qs if kind else kv]
        at = 3 + kind
        return copy(place, place, f_send.at[at, owner], f_recv.at[at, owner], {"grp": twin})

    def sides(k, act):
        @pl.when(s >= k)
        def _():
            act(s - k, True, s < count - 1)

        @pl.when(s + k < count)
        def _():
            act(s + k, False, s > 0)

    def both_ways(act):
        @pl.when(s < count - 1)
        def _():
            act(True)

        @pl.when(s > 0)
        def _():
            act(False)

    local[0].wait()
    both_ways(lambda up: z_copy(0, s, up).start())
    local[1].wait()
    local[2].wait()
    both_ways(lambda up: z_copy(1, s, up).start())
    for off in order:
        q_copy(off).start()

    def norm_block(owner):
        step = 16

        def one(i, carry):
            at = pl.ds(pl.multiple_of(owner * rows + i * step, step), step)
            x = tok_all[at, :].astype(f32)
            scale = lax.rsqrt(jnp.mean(x * x, axis=-1, keepdims=True) + epsilon)
            norm_all[at, :] = (x * scale * gain[...]).astype(bf16)
            return carry

        lax.fori_loop(0, rows // step, one, 0)

    def z_tok(owner, up, more):
        z_copy(0, owner, True).wait_recv()

        @pl.when(more)
        def _():
            z_copy(0, owner, up).start()

        tok_forward(1, owner).start()
        tok_forward(0, owner).start()

    def z_weight(owner, up, more):
        z_copy(1, owner, True).wait_recv()

        @pl.when(more)
        def _():
            z_copy(1, owner, up).start()

        w_forward(0, owner).start()
        q_arrival(owner).wait_recv()
        w_forward(1, owner).start()

    def x_tok(owner, up, more):
        tok_forward(1, owner).wait_recv()
        tok_forward(2, owner).start()

    def norm_owner(owner, up, more):
        tok_forward(0, owner).wait_recv()
        tok_forward(2, owner).wait_recv()
        norm_block(owner)

    norm_block(s)
    last = count - 1
    for k in range(1, count):
        sides(k, z_tok)
        if k > 1:
            sides(k - 1, x_tok)
        if k > 2:
            sides(k - 2, norm_owner)
        sides(k, z_weight)
    if last > 1:
        sides(last - 1, norm_owner)
    sides(last, x_tok)
    sides(last, norm_owner)

    seq = rows * count
    group = wpo.shape[0]
    window = jnp.where(t == 0, 2, jnp.where(t == 1, 4, jnp.where(t == 2, 8, 16)))
    half_span = window // 2

    def pool(b, carry):
        at = b * rows + lax.broadcasted_iota(jnp.int32, (rows, seq), 0)
        col = lax.broadcasted_iota(jnp.int32, (rows, seq), 1)
        inside = (col >= at - half_span) & (col < at + window - half_span)
        band = jnp.where(inside, 1.0, 0.0).astype(bf16)
        total = jnp.dot(band, norm_all[:, span(t, group)], preferred_element_type=f32)
        pos = b * rows + lax.broadcasted_iota(jnp.int32, (rows, 1), 0)
        low = jnp.maximum(pos - half_span, 0)
        high = jnp.minimum(pos + window - half_span, seq)
        own = norm_all[span(b, rows), span(t, group)].astype(f32)
        pooled_all[span(b, rows), :] = (total / (high - low).astype(f32) - own).astype(bf16)
        return carry

    lax.fori_loop(0, count, pool, 0)

    def y_arrival(owner, up, more):
        w_forward(0, owner).wait_recv()
        w_forward(1, owner).wait_recv()

    for k in range(1, count):
        sides(k, y_arrival)
    local[3].wait()

    def project(b, carry):
        acc = jnp.dot(norm_all[span(b, rows), :], w_all[...], preferred_element_type=f32)
        k_all[span(b, rows), :] = acc[:, 0:LANES].astype(bf16)
        v_all[span(b, rows), :] = acc[:, LANES : 2 * LANES].astype(bf16)
        q_all[span(b, rows), :] = acc[:, 2 * LANES : 3 * LANES].astype(bf16)
        return carry

    lax.fori_loop(0, count, project, 0)

    def head_copy(b, off):
        place = heads_all.at[span(b, rows), span(s, LANES)]
        peer = lax.rem(s + off, count)
        return copy(place, place, h_send.at[b, off], h_recv.at[b, off], {"sp": peer})

    def lt_copy(b):
        return copy(lt_send.at[b], lt_in.at[s], l_send.at[b], l_recv.at[s], {"sp": b})

    lane = lax.broadcasted_iota(jnp.int32, (rows, LANES), 1)
    lt_rows = lt_send.shape[2]

    def attend(b, carry):
        q = q_all[span(b, rows), :]
        reads, logs = [], []
        for m in range(2):
            q_m = jnp.where((lane >= HD) == (m == 1), q, jnp.zeros_like(q))
            scores = (
                lax.dot_general(
                    q_m, k_all[...], (((1,), (1,)), ((), ())), preferred_element_type=f32
                )
                * HD ** (-0.5)
            )
            highest = jnp.max(scores, axis=-1, keepdims=True)
            weights = jnp.exp(scores - highest)
            totals = jnp.sum(weights, axis=-1, keepdims=True)
            reads.append(
                jnp.dot(weights.astype(bf16), v_all[...], preferred_element_type=f32) / totals
            )
            logs.append(highest + jnp.log(totals))
        contrast = reads[0] - lam[s] * reads[1]
        scaled = (
            contrast
            * lax.rsqrt(jnp.mean(contrast * contrast, axis=-1, keepdims=True) + epsilon)
            * hgain[pl.ds(s, 1), :]
        )
        heads_all[span(b, rows), span(s, LANES)] = scaled.astype(bf16)
        for off in order:
            head_copy(b, off).start()
        both = jnp.where(lane == 0, logs[0], logs[1])
        padded = jnp.concatenate([both, jnp.zeros((lt_rows - rows, LANES), f32)], axis=0)
        lt_send[b] = jnp.transpose(padded)[0:8, :]

        @pl.when(b != s)
        def _():
            lt_copy(b).start()

        return carry

    lax.fori_loop(0, count, attend, 0)

    sub = rows // 4
    peers = (sib, far, diag)

    def part_copy(b, j):
        return copy(
            part_out.at[b, peers[j]],
            part_in.at[b, j],
            p_send.at[b, j],
            p_recv.at[b, j],
            {"tp": peers[j]},
        )

    local[4].wait()
    local[5].wait()

    def out_copy(b):
        return copy(block_out.at[b], block_in.at[s], o_send.at[b], o_recv.at[s], {"sp": b})

    def finish(b):
        total = part_out[b, t].astype(f32)
        for j in range(3):
            part_copy(b, j).wait_recv()
            total = total + part_in[b, j].astype(f32)
        block_out[b] = total.astype(bf16)

        @pl.when(b != s)
        def _():
            out_copy(b).start()

    def outward(b, carry):
        for off in order:
            head_copy(b, off).wait_recv()
        total = jnp.dot(heads_all[span(b, rows), :], wao_in[...], preferred_element_type=f32)
        total = total + jnp.dot(
            pooled_all[span(b, rows), :], wpo_in[...], preferred_element_type=f32
        )
        for j in range(4):
            part_out[b, j] = total[j * sub : (j + 1) * sub, :].astype(bf16)
        for j in (2, 1, 0):
            part_copy(b, j).start()

        @pl.when(b > 0)
        def _():
            finish(b - 1)

        return carry

    lax.fori_loop(0, count, outward, 0)

    finish(count - 1)

    def put_logs(b, ref):
        for m in range(2):
            lt_out[m, b : b + 1, :] = ref[b, m : m + 1, 0:rows]

    for b in range(count):
        cols = slice(b * group, (b + 1) * group)

        @pl.when(s == b)
        def _():
            mixed_out[:, cols] = block_out[b]
            put_logs(b, lt_send)

        @pl.when(s != b)
        def _():
            copy(
                block_out.at[s], block_in.at[b], o_send.at[s], o_recv.at[b], {"sp": b}
            ).wait_recv()
            copy(lt_send.at[s], lt_in.at[b], l_send.at[s], l_recv.at[b], {"sp": b}).wait_recv()
            mixed_out[:, cols] = block_in[b]
            put_logs(b, lt_in)
            out_copy(b).wait_send()
            lt_copy(b).wait_send()

    both_ways(lambda up: z_copy(0, s, up).wait_send())
    both_ways(lambda up: z_copy(1, s, up).wait_send())
    for off in order:
        q_copy(off).wait_send()

    def sent(owner, up, more):
        @pl.when(more)
        def _():
            z_copy(0, owner, up).wait_send()
            z_copy(1, owner, up).wait_send()

        for step in range(3):
            tok_forward(step, owner).wait_send()
        w_forward(0, owner).wait_send()
        w_forward(1, owner).wait_send()

    for k in range(1, count):
        sides(k, sent)

    def drain(b, carry):
        for off in order:
            head_copy(b, off).wait_send()
        for j in range(3):
            part_copy(b, j).wait_send()
        return carry

    lax.fori_loop(0, count, drain, 0)


def fused(
    count,
    tokens,
    norm_gain,
    query_weight,
    key_weight,
    value_weight,
    map_lambda,
    head_gain,
    attn_out_weight,
    pool_out_weight,
):
    rows, width = tokens.shape
    cols = attn_out_weight.shape[1]
    sub = rows // 4
    seq = rows * count
    lt_rows = -(-rows // LANES) * LANES
    bf16, f32 = jnp.bfloat16, jnp.float32
    vmem = pl.BlockSpec(memory_space=pltpu.VMEM)
    smem = pl.BlockSpec(memory_space=pltpu.SMEM)
    far = pl.BlockSpec(memory_space=pl.ANY)
    sems = pltpu.SemaphoreType.DMA
    return pl.pallas_call(
        functools.partial(fused_kernel, count),
        out_shape=(
            jax.ShapeDtypeStruct((sub, width), bf16),
            jax.ShapeDtypeStruct((2, count, rows), f32),
        ),
        in_specs=[far, vmem, far, far, far, smem, vmem, far, far],
        out_specs=(vmem, vmem),
        scratch_shapes=[
            pltpu.VMEM((seq, width), bf16),
            pltpu.VMEM((seq, width), bf16),
            pltpu.VMEM((width, 3 * LANES), bf16),
            pltpu.VMEM((seq, LANES), bf16),
            pltpu.VMEM((seq, LANES), bf16),
            pltpu.VMEM((seq, LANES), bf16),
            pltpu.VMEM((seq, count * LANES), bf16),
            pltpu.VMEM((seq, pool_out_weight.shape[0]), bf16),
            pltpu.VMEM((count, 4, sub, cols), bf16),
            pltpu.VMEM((count, 3, sub, cols), bf16),
            pltpu.VMEM((count, sub, cols), bf16),
            pltpu.VMEM((count, sub, cols), bf16),
            pltpu.VMEM((count, 8, lt_rows), f32),
            pltpu.VMEM((count, 8, lt_rows), f32),
            pltpu.VMEM(attn_out_weight.shape, bf16),
            pltpu.VMEM(pool_out_weight.shape, bf16),
            sems((6,)),
            sems((count,)),
            sems((count,)),
            sems((2, count, 2)),
            sems((2, count)),
            sems((5, count)),
            sems((5, count)),
            sems((count, count)),
            sems((count, count)),
            sems((count, 3)),
            sems((count, 3)),
            sems((count,)),
            sems((count,)),
            sems((count,)),
            sems((count,)),
        ],
        compiler_params=pltpu.CompilerParams(collective_id=0, has_side_effects=True),
    )(
        tokens,
        norm_gain.reshape(1, width),
        query_weight,
        key_weight,
        value_weight,
        map_lambda,
        head_gain,
        attn_out_weight,
        pool_out_weight,
    )


def fits(shape, tokens, query_weight, value_weight, map_lambda, pool_out_weight):
    count = shape["sp"]
    return (
        shape["grp"] == 2
        and shape["tp"] == 4
        and count > 1
        and map_lambda.shape[0] == count
        and value_weight.shape[1] == VD == LANES == 2 * HD
        and tokens.shape[0] % 32 == 0
        and tokens.shape[1] % (4 * LANES) == 0
        and query_weight.shape[0] % 32 == 0
        and pool_out_weight.shape[0] * 4 == tokens.shape[1]
        and pool_out_weight.shape[1] % LANES == 0
        and pool_out_weight.shape[1] * count == tokens.shape[1]
        and pool_out_weight.shape[0] == pool_out_weight.shape[1]
        and tokens.shape[0] * count * tokens.shape[1] <= 1 << 22
    )


def solution(mesh):
    placed = (
        P(("grp", "sp"), None),
        P(),
        P("sp", "tp"),
        P("sp", "tp"),
        P("sp", "tp"),
        P("tp"),
        P("tp", None),
        P("tp", "sp"),
        P("tp", "sp"),
    )
    shape = dict(mesh.shape)

    def chosen(*args):
        if fits(shape, args[0], args[2], args[4], args[5], args[8]):
            return fused(shape["sp"], *args)
        return on_device(*args)

    return jax.shard_map(
        chosen,
        mesh=mesh,
        in_specs=placed,
        out_specs=(P(("grp", "sp", "tp"), None), P(None, "tp", ("grp", "sp"))),
        check_vma=False,
    )
```
